512 devices in a mesh: sp: 64 (over z, y), tp: 8 (over x, core).
Axes of the slice: x: 4, y: 8, z: 8, core: 2. Of those that a mesh axis runs over, the one named last changes fastest.
Arguments:
- tokens: bfloat16 [8192, 2048], P('sp'), may hold values from -6 to 6
- norm_gain: float32 [2048], replicated, may hold values from 0.1 to 1.9
- conv_value_weight: bfloat16 [2048, 1024], P('sp', 'tp'), may hold values from -0.125 to 0.125
- conv_gate_weight: bfloat16 [2048, 1024], P('sp', 'tp'), may hold values from -0.125 to 0.125
- conv_kernel: float32 [31, 1024], P(None, 'tp'), may hold values from -10 to 10
- conv_bias: float32 [1024], P('tp'), may hold values from -4 to 4
- channel_gain: float32 [1024], P('tp'), may hold values from 0.1 to 1.9
- query_weight: bfloat16 [2048, 2048], P('sp', 'tp'), may hold values from -0.125 to 0.125
- key_weight: bfloat16 [2048, 2048], P('sp', 'tp'), may hold values from -0.125 to 0.125
- value_weight: bfloat16 [2048, 4096], P('sp', 'tp'), may hold values from -0.125 to 0.125
- gate_weight: bfloat16 [2048, 32], replicated, may hold values from -0.125 to 0.125
- gate_offset: float32 [2, 2, 8, 8192], P(None, None, 'tp', 'sp'), may hold values from -110 to 160, as said below
- start_memory: float32 [2, 8, 512, 256], P(None, 'tp'), may hold values from -0.375 to 0.375
- start_norm: float32 [2, 8, 256], P(None, 'tp'), may hold values from -0.375 to 0.375
- start_level: float32 [2, 8], P(None, 'tp'), may hold values from 2 to 5
- cell_gain: float32 [4096], P('tp'), may hold values from 0.1 to 1.9
- out_conv_weight: bfloat16 [2048, 1024], P('sp', 'tp'), may hold values from -0.25 to 0.25
- out_cell_weight: bfloat16 [2048, 4096], P('sp', 'tp'), may hold values from -0.09375 to 0.09375
Outputs:
- mixed: bfloat16 [8192, 2048], P(('sp', 'tp'))
The draws below stay inside these ranges and needn't reach their ends.
Inputs may be any that keep to these rules, and one draw needn't show every extreme that they name: `gate_offset`: added to the gate pre-activations; index 0 of the second dimension is the input gate, index 1 the forget gate.
All inputs are finite; a program needn't handle non-finite values.
Results may differ from the reference program's by a relative error of at most 0.017.
Values may be sent and summed in bfloat16 or wider, within the bound.
No kernel may reach another device: no remote copies, remote signals or barrier semaphores. Data moves between devices by JAX's collectives and lax.ppermute only.
A program may use at most 128 MiB of HBM per device.

```python
import math
import jax
import jax.numpy as jnp
from jax import lax

D = 2048
CONV_W = 1024
MEMORY_GROUPS = 8
KEY_DIM = 256
VALUE_DIM = 512
KERNEL = 31
BLOCK = 128
TOK_DEV = 128
STEP_COUNT = 8192
N_TP = 8


def draw_conv_kernel(key, part):
    base_key, rough_key = jax.random.split(jax.random.fold_in(key, 11))
    channel = jnp.arange(CONV_W, dtype=jnp.float32) / CONV_W
    roughness = jnp.exp(jax.random.uniform(rough_key, (CONV_W,), minval=-0.5, maxval=0.5))
    channel_scale = jnp.exp(math.log(8.0) * channel)
    entries = jnp.clip(jax.random.normal(base_key, (KERNEL, CONV_W)), -4.0, 4.0)
    return (entries * channel_scale * roughness / math.sqrt(KERNEL)).astype(jnp.float32)


def draw_gate_offset(key, part):
    frequency_seed, permute_seed, surge_seed, feature_seed = jax.random.split(jax.random.fold_in(key, 23), 4)
    step_index = jnp.arange(STEP_COUNT)
    device_block = step_index // TOK_DEV
    device_count = STEP_COUNT // TOK_DEV
    device_rate = jnp.exp(jax.random.uniform(frequency_seed, (2, MEMORY_GROUPS, device_count), minval=math.log(0.4), maxval=math.log(2.5)))
    rate_here = jnp.take(device_rate, device_block, axis=2)
    order_keys = jax.random.split(permute_seed, 2)
    head_rank = jnp.stack([jax.random.permutation(order_keys[0], MEMORY_GROUPS), jax.random.permutation(order_keys[1], MEMORY_GROUPS)])
    fast_count = MEMORY_GROUPS // 2
    slow_level = jnp.log(2.0 * STEP_COUNT / rate_here)
    input_part = jnp.clip(jax.random.normal(feature_seed, (2, MEMORY_GROUPS, STEP_COUNT)), -4.0, 4.0)
    fast_head = (head_rank < fast_count)[:, :, None]
    surge_index = jax.random.randint(surge_seed, (2, MEMORY_GROUPS, 2), 0, STEP_COUNT)
    surge_flags = jnp.any(step_index[None, None, None, :] == surge_index[:, :, :, None], axis=2)
    decay_fraction = jnp.where(fast_head, 3.2, slow_level)
    decay_fraction = jnp.where(surge_flags, 0.5, decay_fraction)
    return jnp.stack([input_part, decay_fraction], axis=1).astype(jnp.float32)


def steps_of(stream_key, dims, pieces, smallest, largest):
    def one(dim, shards_of):
        heights = jax.random.uniform(jax.random.fold_in(jax.random.fold_in(stream_key, 6), dim), (shards_of,), jnp.float32, smallest / len(pieces), largest / len(pieces))
        return jnp.repeat(jnp.exp(heights), dims[dim] // shards_of).reshape((-1,) + (1,) * (len(dims) - dim - 1))

    gain = one(*pieces[0])
    for cut in pieces[1:]:
        gain = gain * one(*cut)
    return gain


def centred(stream_key, extent, scale, bound, cuts=(), kind=jnp.bfloat16):
    gain = steps_of(stream_key, extent, cuts, -0.22, 0.18) if cuts else 1.0
    values = jax.random.normal(stream_key, extent, jnp.float32) * scale * gain
    return jnp.minimum(jnp.maximum(values, -bound), bound).astype(kind)


def setup_inputs(seed: int = 0) -> dict:
    seeds = jax.random.split(jax.random.key(seed), 19)
    tokens = centred(seeds[0], (STEP_COUNT, D), 1.0, 6.0, ((0, 64),))
    norm_gain = jnp.clip(1.0 + 0.18 * jax.random.normal(seeds[1], (D,), jnp.float32), 0.1, 1.9)
    conv_value_weight = centred(seeds[2], (D, CONV_W), D ** -0.5, 0.125, ((0, 64), (1, 8)))
    conv_gate_weight = centred(seeds[3], (D, CONV_W), D ** -0.5, 0.125, ((0, 64), (1, 8)))
    conv_kernel = draw_conv_kernel(jax.random.fold_in(seeds[18], 71), 0)
    conv_bias = centred(seeds[5], (CONV_W,), 1.0, 4.0, ((0, 8),), jnp.float32)
    channel_gain = jnp.clip(1.0 + 0.18 * jax.random.normal(seeds[6], (CONV_W,), jnp.float32), 0.1, 1.9)
    query_weight = centred(seeds[7], (D, MEMORY_GROUPS * KEY_DIM), D ** -0.5, 0.125, ((0, 64), (1, 8)))
    key_weight = centred(seeds[8], (D, MEMORY_GROUPS * KEY_DIM), D ** -0.5, 0.125, ((0, 64), (1, 8)))
    value_weight = centred(seeds[9], (D, MEMORY_GROUPS * VALUE_DIM), D ** -0.5, 0.125, ((0, 64), (1, 8)))
    gate_weight = centred(seeds[10], (D, 4 * MEMORY_GROUPS), D ** -0.5, 0.125)
    gate_offset = draw_gate_offset(jax.random.fold_in(seeds[18], 71), 0)
    start_memory = centred(seeds[12], (2, MEMORY_GROUPS, VALUE_DIM, KEY_DIM), KEY_DIM ** -0.5, 0.375, ((1, 8),), jnp.float32)
    start_norm = centred(seeds[13], (2, MEMORY_GROUPS, KEY_DIM), KEY_DIM ** -0.5, 0.375, ((1, 8),), jnp.float32)
    start_level = jnp.clip(2.0 + 3.0 * jax.random.uniform(seeds[14], (2, MEMORY_GROUPS), jnp.float32) ** steps_of(seeds[14], (2, MEMORY_GROUPS), ((1, 8),), -0.2, 0.2), 2.0, 5.0)
    cell_gain = jnp.clip(1.0 + 0.18 * jax.random.normal(seeds[15], (MEMORY_GROUPS * VALUE_DIM,), jnp.float32), 0.1, 1.9)
    out_conv_weight = centred(seeds[16], (D, CONV_W), (CONV_W // 2) ** -0.5, 0.25, ((0, 64), (1, 8)))
    out_cell_weight = centred(seeds[17], (D, MEMORY_GROUPS * VALUE_DIM), (MEMORY_GROUPS * VALUE_DIM) ** -0.5, 0.09375, ((0, 64), (1, 8)))
    return {"tokens": tokens, "norm_gain": norm_gain, "conv_value_weight": conv_value_weight, "conv_gate_weight": conv_gate_weight, "conv_kernel": conv_kernel, "conv_bias": conv_bias, "channel_gain": channel_gain, "query_weight": query_weight, "key_weight": key_weight, "value_weight": value_weight, "gate_weight": gate_weight, "gate_offset": gate_offset, "start_memory": start_memory, "start_norm": start_norm, "start_level": start_level, "cell_gain": cell_gain, "out_conv_weight": out_conv_weight, "out_cell_weight": out_cell_weight}


EPS = 1e-06
HIGHEST = lax.Precision.HIGHEST

def back_to_wide(values):
    return lax.optimization_barrier(values.astype(jnp.bfloat16)).astype(jnp.float32)

def block_step(carried, inputs):
    memory, normer, run_level = carried
    queries, key_rows, value_rows, in_gate, log_forget = inputs
    length = queries.shape[0]
    lower_mask = jnp.arange(length)[:, None] >= jnp.arange(length)[None, :]
    cumulative = jnp.cumsum(log_forget)
    decay_table = jnp.where(lower_mask, cumulative[:, None] - cumulative[None, :] + in_gate[None, :], -jnp.inf)
    carried_level = cumulative + run_level
    top_level = jnp.maximum(carried_level, lax.optimization_barrier(jnp.max(decay_table, axis=1)))
    carry_weight = jnp.exp(carried_level - top_level)
    scores = jnp.dot(queries, key_rows.T, precision=HIGHEST) * jnp.exp(decay_table - top_level[:, None])
    numerator = jnp.dot(scores, value_rows, precision=HIGHEST) + carry_weight[:, None] * jnp.dot(queries, memory.T, precision=HIGHEST)
    denominator = lax.optimization_barrier(jnp.sum(scores, axis=1)) + carry_weight * jnp.dot(queries, normer, precision=HIGHEST)
    outputs = numerator / jnp.maximum(jnp.abs(denominator), 1.0)[:, None]
    block_total = cumulative[-1]
    tail_level = block_total - cumulative + in_gate
    new_level = jnp.maximum(block_total + run_level, jnp.max(tail_level))
    old_weight = jnp.exp(block_total + run_level - new_level)
    new_weight = jnp.exp(tail_level - new_level)
    memory = old_weight * memory + jnp.dot((value_rows * new_weight[:, None]).T, key_rows, precision=HIGHEST)
    normer = old_weight * normer + jnp.dot(new_weight, key_rows, precision=HIGHEST)
    return ((memory, normer, new_level), outputs)

def run_cell(queries, key_rows, value_rows, in_gate, log_forget, memory, normer, run_level):
    blocks = queries.shape[0] // BLOCK

    def to_blocks(values):
        return values.reshape((blocks, BLOCK) + values.shape[1:])
    final_state, outputs = lax.scan(block_step, (memory, normer, run_level), tuple((to_blocks(values) for values in (queries, key_rows, value_rows, in_gate, log_forget))))
    return outputs.reshape(queries.shape[0], value_rows.shape[1])

def head_outputs(inputs):
    queries, key_rows, value_rows, in_gate, log_forget, memory, normer, run_level = inputs
    forward = run_cell(queries, key_rows, value_rows, in_gate[0], log_forget[0], memory[0], normer[0], run_level[0])
    backward = run_cell(queries[::-1], key_rows[::-1], value_rows[::-1], in_gate[1, ::-1], log_forget[1, ::-1], memory[1], normer[1], run_level[1])[::-1]
    both_ways = forward + backward
    return both_ways * lax.rsqrt(lax.optimization_barrier(jnp.mean(both_ways * both_ways, axis=1, keepdims=True)) + EPS)

def reference(tokens, norm_gain, conv_value_weight, conv_gate_weight, conv_kernel, conv_bias, channel_gain, query_weight, key_weight, value_weight, gate_weight, gate_offset, start_memory, start_norm, start_level, cell_gain, out_conv_weight, out_cell_weight):
    features = tokens.astype(jnp.float32)
    normed = (features * lax.rsqrt(lax.optimization_barrier(jnp.mean(features * features, axis=1, keepdims=True)) + EPS) * norm_gain).astype(jnp.bfloat16)

    def project(weight):
        return jnp.dot(normed, weight, preferred_element_type=jnp.float32)
    conv_value = project(conv_value_weight).astype(jnp.bfloat16)
    conv_gate = project(conv_gate_weight).astype(jnp.bfloat16)
    gated_rows = (conv_value.astype(jnp.float32) * jax.nn.sigmoid(conv_gate.astype(jnp.float32))).astype(jnp.bfloat16)
    half_reach = KERNEL // 2
    padded = jnp.pad(gated_rows.astype(jnp.float32), ((half_reach, half_reach), (0, 0)))
    conv_sum = conv_bias + sum((conv_kernel[offset] * padded[offset:offset + STEP_COUNT] for offset in range(KERNEL)))
    channel_mean = lax.optimization_barrier(jnp.mean(conv_sum, axis=1, keepdims=True))
    channel_var = lax.optimization_barrier(jnp.mean(conv_sum * conv_sum, axis=1, keepdims=True)) - channel_mean * channel_mean
    conv_out = jax.nn.silu((conv_sum - channel_mean) * lax.rsqrt(channel_var + EPS) * channel_gain).astype(jnp.bfloat16)

    def split_heads(flat_rows, head_width):
        return jnp.transpose(back_to_wide(flat_rows).reshape(STEP_COUNT, MEMORY_GROUPS, head_width), (1, 0, 2))
    queries = split_heads(project(query_weight), KEY_DIM)
    key_rows = split_heads(project(key_weight), KEY_DIM) * KEY_DIM ** (-0.5)
    value_rows = split_heads(project(value_weight), VALUE_DIM)
    gate_pre = project(gate_weight).reshape(STEP_COUNT, 2, 2, MEMORY_GROUPS)
    gate_pre = jnp.transpose(gate_pre, (1, 2, 3, 0)) + gate_offset
    in_gate = jnp.transpose(gate_pre[:, 0], (1, 0, 2))
    log_forget = jnp.transpose(jax.nn.log_sigmoid(gate_pre[:, 1]), (1, 0, 2))
    cells = lax.map(head_outputs, (queries, key_rows, value_rows, in_gate, log_forget, jnp.transpose(start_memory, (1, 0, 2, 3)), jnp.transpose(start_norm, (1, 0, 2)), jnp.transpose(start_level, (1, 0))))
    cell_out = (jnp.transpose(cells, (1, 0, 2)).reshape(STEP_COUNT, MEMORY_GROUPS * VALUE_DIM) * cell_gain).astype(jnp.bfloat16)
    conv_groups = conv_out.reshape(STEP_COUNT, N_TP, CONV_W // N_TP)
    cell_groups = cell_out.reshape(STEP_COUNT, N_TP, MEMORY_GROUPS * VALUE_DIM // N_TP)
    conv_weights = out_conv_weight.reshape(D, N_TP, CONV_W // N_TP)
    cell_weights = out_cell_weight.reshape(D, N_TP, MEMORY_GROUPS * VALUE_DIM // N_TP)
    mixed_sum = jnp.zeros((STEP_COUNT, D), jnp.float32)
    for group in range(N_TP):
        partial_value = jnp.einsum('tc,dc->td', conv_groups[:, group], conv_weights[:, group], preferred_element_type=jnp.float32) + jnp.einsum('tc,dc->td', cell_groups[:, group], cell_weights[:, group], preferred_element_type=jnp.float32)
        mixed_sum = mixed_sum + lax.optimization_barrier(partial_value.astype(jnp.bfloat16)).astype(jnp.float32)
    return mixed_sum.astype(jnp.bfloat16)
```

```python
import jax
import jax.numpy as jnp
from jax import lax
from jax.experimental import pallas as pl
from jax.experimental.pallas import tpu as pltpu
from jax.sharding import Mesh
from jax.sharding import PartitionSpec as P

SP = ("z", "y")
TP = ("x", "c")
EPS = 1e-06
LOW = -1e30
BF = jnp.bfloat16
F32 = jnp.float32


def to_each(value, axis):
    count = lax.axis_size(axis)
    return lax.all_to_all(
        jnp.broadcast_to(value[None], (count, *value.shape)), axis, 0, 0, tiled=True
    )


def side_by_side(arrays):
    widths = [a.shape[1] for a in arrays]

    def body(*refs):
        out, at = refs[-1], 0
        for ref, width in zip(refs[:-1], widths):
            out[:, at : at + width] = ref[...]
            at += width

    return pl.pallas_call(
        body,
        out_shape=jax.ShapeDtypeStruct((arrays[0].shape[0], sum(widths)), arrays[0].dtype),
    )(*arrays)


def norm_rows(tokens, gain):
    features = tokens.astype(F32)
    scale = lax.rsqrt(jnp.mean(features * features, axis=1, keepdims=True) + EPS)
    return (features * scale * gain).astype(BF)


def group_tokens(normed, t):
    rows, width = normed.shape
    share = rows // lax.axis_size(TP)
    piece = lax.dynamic_slice_in_dim(normed, t * share, share, 0)
    found = to_each(piece, "y")
    found = to_each(found, "x")
    found = to_each(found, "c")
    found = jnp.transpose(found, (2, 1, 0, 3, 4))
    return found.reshape(-1, width)


def levels(gates, start_level, z, d, per_group):
    chunks, _, rows = gates.shape
    groups = chunks // per_group
    in_gate, forget = gates[:, 0], gates[:, 1]
    p = jnp.arange(rows)
    c = jnp.arange(chunks)
    before = (lambda a, b: a < b) if d == 0 else (lambda a, b: a > b)
    upto = before(p[None, :], p[:, None]) | (p[None, :] == p[:, None])
    cum = jnp.sum(jnp.where(upto[None], forget[:, None, :], 0.0), axis=2)
    total = jnp.sum(forget, axis=1)
    first = in_gate - cum
    tail = total[:, None] - cum + in_gate
    level = jnp.max(tail, axis=1)
    between = before(c[:, None, None], c[None, None, :]) & before(c[None, None, :], c[None, :, None])
    gap = jnp.sum(jnp.where(between, total[None, None, :], 0.0), axis=2)
    earlier = before(c[:, None], c[None, :])
    lead = jnp.sum(jnp.where(earlier, total[:, None], 0.0), axis=0)
    enter = jnp.maximum(
        start_level + lead, jnp.max(jnp.where(earlier, level[:, None] + gap, LOW), axis=0)
    )
    group = c // per_group
    same = group[:, None] == group[None, :]
    rest = jnp.sum(jnp.where(same & before(c[:, None], c[None, :]), total[None, :], 0.0), axis=1)
    group_level = jnp.max((level + rest).reshape(groups, per_group), axis=1)
    g = jnp.arange(groups)
    door = z * per_group + (0 if d == 0 else per_group - 1)
    enter_door = jnp.sum(jnp.where(c == door, enter, 0.0))
    lead_door = jnp.sum(jnp.where(c == door, lead, 0.0))
    middle = before(g[:, None], group[None, :]) & before(group[None, :], z)
    group_gap = jnp.sum(jnp.where(middle, total[None, :], 0.0), axis=1)
    coef = jnp.where(
        before(g, z), jnp.exp(jnp.where(before(g, z), group_level + group_gap - enter_door, LOW)), 0.0
    )
    start_coef = jnp.exp(start_level + lead_door - enter_door)

    def own(values):
        return lax.dynamic_slice_in_dim(values, z * per_group, per_group, 0)

    def own2(values):
        return lax.dynamic_slice(
            values, (z * per_group, z * per_group), (per_group, per_group)
        )

    first_own, tail_own, enter_own = own(first), own(tail), own(enter)
    peak = jnp.max(jnp.where(upto[None], first_own[:, None, :], LOW), axis=2)
    top = jnp.maximum(enter_own[:, None], peak)
    o = jnp.arange(per_group)
    from_door = jnp.sum(
        jnp.where(before(o[:, None], o[None, :]), own(total)[:, None], 0.0), axis=0
    )
    entry = jnp.exp((from_door + enter_door)[:, None] - top)
    own_group = jnp.sum(jnp.where(g == z, group_level, 0.0))
    state_weight = jnp.exp(tail_own + own(rest)[:, None] - own_group)
    seen = jnp.where(
        before(o[:, None], o[None, :])[:, :, None],
        tail_own[:, None, :] + own2(gap)[:, :, None],
        jnp.where((o[:, None] == o[None, :])[:, :, None], first_own[:, None, :], LOW),
    )
    seen = jnp.transpose(seen, (1, 0, 2)).reshape(per_group, per_group * rows)
    return seen, top.reshape(-1), entry.reshape(-1), state_weight.reshape(-1), coef, start_coef


def pair_weights(seen, top, d):
    per_group, length = seen.shape
    rows = length // per_group
    t = jnp.arange(length)
    order = (t[None, :] <= t[:, None]) if d == 0 else (t[None, :] >= t[:, None])
    expo = jnp.broadcast_to(seen[:, None, :], (per_group, rows, length)).reshape(length, length)
    return jnp.where(order, jnp.exp(jnp.where(order, expo - top[:, None], LOW)), 0.0)


def shards(
    tokens,
    norm_gain,
    conv_value_weight,
    conv_gate_weight,
    conv_kernel,
    conv_bias,
    channel_gain,
    query_weight,
    key_weight,
    value_weight,
    gate_weight,
    gate_offset,
    start_memory,
    start_norm,
    start_level,
    cell_gain,
    out_conv_weight,
    out_cell_weight,
):
    z, y, t = lax.axis_index("z"), lax.axis_index("y"), lax.axis_index(TP)
    z_count, y_count, t_count = lax.axis_size("z"), lax.axis_size("y"), lax.axis_size(TP)
    rows = tokens.shape[0]
    chan = conv_kernel.shape[1]
    key_width = start_norm.shape[2]
    value_width = start_memory.shape[2]
    share = value_width // y_count
    channels = chan * t_count

    weights = side_by_side(
        (
            conv_value_weight,
            conv_gate_weight,
            query_weight,
            key_weight,
            value_weight,
            out_conv_weight,
            out_cell_weight,
        )
    )
    weights = lax.all_gather(weights, SP, axis=0, tiled=True)
    at = 2 * chan + 2 * key_width
    conv_weights = weights[:, : 2 * chan]
    query_key_weights = weights[:, 2 * chan : at]
    value_weights = weights[:, at : at + value_width]
    out_weights = weights[:, at + value_width :]

    normed = norm_rows(tokens, norm_gain)

    heads = gate_weight.shape[1] // 4
    gate_pre = jnp.dot(normed, gate_weight, preferred_element_type=F32)
    mine = jnp.arange(heads) == t
    gate_pre = jnp.sum(
        jnp.where(mine, gate_pre.reshape(rows, 4, heads), 0.0), axis=2
    ).T.reshape(2, 2, rows)
    gate_pre = gate_pre + gate_offset[:, :, 0]
    gates = jnp.stack([gate_pre[:, 0], jax.nn.log_sigmoid(gate_pre[:, 1])], axis=1)
    gates = to_each(gates.reshape(4, rows), SP).reshape(-1, 2, 2, rows)

    half = conv_kernel.shape[0] // 2
    pad = 16
    count = z_count * y_count
    up = [(i, i + 1) for i in range(count - 1)]
    down = [(i + 1, i) for i in range(count - 1)]
    above = lax.ppermute(normed[rows - pad :], SP, up)
    below = lax.ppermute(normed[:pad], SP, down)
    around = jnp.concatenate([above, normed, below], axis=0)

    group = group_tokens(normed, t)
    plans = [levels(gates[:, d], start_level[d, 0], z, d, y_count) for d in range(2)]

    query_key = jnp.dot(group, query_key_weights, preferred_element_type=F32).astype(BF)
    queries = query_key[:, :key_width]
    key_rows = query_key[:, key_width:] * BF(key_width ** (-0.5))
    value_slice = lax.dynamic_slice_in_dim(value_weights, y * share, share, 1)
    value_rows = jnp.dot(group, value_slice, preferred_element_type=F32).astype(BF)

    states = []
    for d in range(2):
        weight = plans[d][3]
        scaled = (value_rows.astype(F32) * weight[:, None]).astype(BF)
        memory = lax.dot_general(
            scaled, key_rows, (((0,), (0,)), ((), ())), preferred_element_type=F32
        )
        normer = jnp.sum(weight[:, None] * key_rows.astype(F32), axis=0)
        high = normer.astype(BF)
        low = (normer - high.astype(F32)).astype(BF)
        states.append(
            jnp.concatenate(
                [memory.astype(BF), high[None], low[None], jnp.zeros((6, key_width), BF)], axis=0
            )
        )
    dest = jnp.arange(z_count)[:, None, None]
    sent = jnp.where(dest > z, states[0][None], states[1][None])
    found = lax.all_to_all(sent, "z", 0, 0, tiled=True).astype(F32)

    conv_both = jnp.dot(around, conv_weights, preferred_element_type=F32).astype(BF).astype(F32)
    gated = (conv_both[:, :chan] * jax.nn.sigmoid(conv_both[:, chan:])).astype(BF).astype(F32)
    shift = pad - half
    conv = conv_bias + sum(
        conv_kernel[j] * gated[shift + j : shift + j + rows] for j in range(conv_kernel.shape[0])
    )
    stats = jnp.stack([jnp.sum(conv, axis=1), jnp.sum(conv * conv, axis=1)])
    stats = jnp.sum(to_each(stats, TP), axis=0) / channels
    mean, var = stats[0], stats[1] - stats[0] * stats[0]
    conv_out = jax.nn.silu(
        (conv - mean[:, None]) * lax.rsqrt(var + EPS)[:, None] * channel_gain
    ).astype(BF)

    scores = lax.dot_general(
        queries, key_rows, (((1,), (1,)), ((), ())), preferred_element_type=F32
    )
    total = 0.0
    for d in range(2):
        seen, top, entry, _, coef, start_coef = plans[d]
        table = scores * pair_weights(seen, top, d)
        state = jnp.sum(coef[:, None, None] * found, axis=0)
        first_memory = lax.dynamic_slice_in_dim(start_memory[d, 0], y * share, share, 0)
        memory = state[:share] + start_coef * first_memory
        normer = state[share] + state[share + 1] + start_coef * start_norm[d, 0]
        high = normer.astype(BF)
        low = (normer - high.astype(F32)).astype(BF)
        carried = jnp.concatenate([memory.astype(BF), high[None], low[None]], axis=0)
        from_state = lax.dot_general(
            queries, carried, (((1,), (1,)), ((), ())), preferred_element_type=F32
        )
        numerator = (
            jnp.dot(table.astype(BF), value_rows, preferred_element_type=F32)
            + entry[:, None] * from_state[:, :share]
        )
        denominator = jnp.sum(table, axis=1) + entry * (
            from_state[:, share] + from_state[:, share + 1]
        )
        total = total + numerator / jnp.maximum(jnp.abs(denominator), 1.0)[:, None]
    cell = total.astype(BF).reshape(y_count, rows, share)
    cell = lax.all_to_all(cell, "y", 0, 0, tiled=True)
    cell = jnp.transpose(cell, (1, 0, 2)).reshape(rows, value_width).astype(F32)
    cell_out = (
        cell * lax.rsqrt(jnp.mean(cell * cell, axis=1, keepdims=True) + EPS) * cell_gain
    ).astype(BF)

    features = jnp.concatenate([conv_out, cell_out], axis=1)
    partial = lax.dot_general(
        features, out_weights, (((1,), (1,)), ((), ())), preferred_element_type=F32
    ).astype(BF)
    partial = lax.all_to_all(
        partial.reshape(t_count, rows // t_count, -1), TP, 0, 0, tiled=True
    )
    return jnp.sum(partial.astype(F32), axis=0).astype(BF)


def solution(mesh):
    z, y, x, c = mesh_shape(mesh)
    split = Mesh(mesh.devices.reshape(z, y, x, c), ("z", "y", "x", "c"))
    return jax.shard_map(
        shards,
        mesh=split,
        in_specs=(
            P(SP, None),
            P(),
            P(SP, TP),
            P(SP, TP),
            P(None, TP),
            P(TP),
            P(TP),
            P(SP, TP),
            P(SP, TP),
            P(SP, TP),
            P(),
            P(None, None, TP, SP),
            P(None, TP, None, None),
            P(None, TP, None),
            P(None, TP),
            P(TP),
            P(SP, TP),
            P(SP, TP),
        ),
        out_specs=P(SP + TP, None),
        check_vma=False,
    )


def mesh_shape(mesh):
    return 8, 8, mesh.shape["tp"] // 2, 2
```

```python
import jax
import jax.numpy as jnp
from jax import lax
from jax.experimental import pallas as pl
from jax.experimental.pallas import tpu as pltpu
from jax.sharding import Mesh
from jax.sharding import PartitionSpec as P


SP = ("z", "y")
TP = ("x", "c")
EPS = 1e-06
LOW = -1e30
BF = jnp.bfloat16
F32 = jnp.float32


def exchange(value, axis):
    return lax.all_to_all(value, axis, 0, 0, tiled=True)


def to_each(value, axis):
    count = lax.axis_size(axis)
    return exchange(jnp.broadcast_to(value[None], (count, *value.shape)), axis)


def side_by_side(arrays):
    widths = [a.shape[1] for a in arrays]

    def body(*refs):
        out, at = refs[-1], 0
        for ref, width in zip(refs[:-1], widths):
            out[:, at : at + width] = ref[...]
            at += width

    return pl.pallas_call(
        body,
        out_shape=jax.ShapeDtypeStruct((arrays[0].shape[0], sum(widths)), arrays[0].dtype),
    )(*arrays)


def own_half(values, parity, share):
    return jnp.where(parity == 1, values[:, share:], values[:, :share])


def states_call(place, query_key, values, columns, share, z_count):
    length, key_width = query_key.shape[0], query_key.shape[1] // 2

    def body(place_ref, qk_ref, value_ref, col_ref, out_ref):
        keys = qk_ref[:, key_width:] * BF(key_width ** (-0.5))
        wide = keys.astype(F32)
        own = own_half(value_ref[...].astype(F32), place_ref[1], share)
        found = []
        for d in range(2):
            weight = col_ref[:, 4 + d : 5 + d]
            memory = lax.dot_general(
                (own * weight).astype(BF),
                keys,
                (((0,), (0,)), ((), ())),
                preferred_element_type=F32,
            ).astype(BF)
            normer = jnp.sum(weight * wide, axis=0, keepdims=True)
            high = normer.astype(BF).astype(F32)
            row = lax.broadcasted_iota(jnp.int32, (16, key_width), 0)
            extra = jnp.where(row == 0, high, jnp.where(row == 1, normer - high, 0.0))
            found.append((memory, extra.astype(BF)))
        for k in range(z_count):

            @pl.when(k > place_ref[0])
            def _():
                out_ref[k, :share, :] = found[0][0]
                out_ref[k, share:, :] = found[0][1]

            @pl.when(k <= place_ref[0])
            def _():
                out_ref[k, :share, :] = found[1][0]
                out_ref[k, share:, :] = found[1][1]

    return pl.pallas_call(
        body,
        in_specs=[
            pl.BlockSpec(memory_space=pltpu.SMEM),
            pl.BlockSpec(memory_space=pltpu.VMEM),
            pl.BlockSpec(memory_space=pltpu.VMEM),
            pl.BlockSpec(memory_space=pltpu.VMEM),
        ],
        out_specs=pl.BlockSpec(memory_space=pltpu.VMEM),
        out_shape=jax.ShapeDtypeStruct((z_count, share + 16, key_width), BF),
        cost_estimate=pl.CostEstimate(
            flops=4 * length * share * key_width, bytes_accessed=2000000, transcendentals=0
        ),
    )(place, query_key, values, columns)


def local_call(place, query_key, values, far, near, columns, share, blocks):
    length, key_width = query_key.shape[0], query_key.shape[1] // 2
    rows = length // blocks
    wide = 256

    def body(place_ref, qk_ref, value_ref, far_ref, near_ref, col_ref, out_ref):
        b = pl.program_id(0)
        here = pl.ds(pl.multiple_of(b * rows, rows), rows)
        scale = BF(key_width ** (-0.5))
        queries = qk_ref[here, :key_width]
        keys = qk_ref[:, key_width:] * scale
        values = own_half(value_ref[...], place_ref[1], share)
        top = [col_ref[here, d : d + 1] for d in range(2)]
        nt = (((1,), (1,)), ((), ()))
        scores = lax.dot_general(queries, keys, nt, preferred_element_type=F32)
        far_row = far_ref[pl.ds(b, 1), :]
        tables = []
        for j in range(blocks):
            part = slice(j * rows, (j + 1) * rows)
            chosen = jnp.where(j < b, top[0], top[1])
            tables.append((scores[:, part] * jnp.exp(far_row[:, part] - chosen)).astype(BF))
        table = jnp.concatenate(tables, axis=1)
        block_of = lax.broadcasted_iota(jnp.int32, (length, 1), 0) // rows
        zero = jnp.zeros_like(values)
        earlier = jnp.where(block_of < b, values, zero)
        later = jnp.where(block_of > b, values, zero)
        lane = lax.broadcasted_iota(jnp.int32, (length, wide - 2 * share), 1)
        ones = jnp.where(
            ((lane == 0) & (block_of < b)) | ((lane == 1) & (block_of > b)), 1.0, 0.0
        ).astype(BF)
        right = jnp.concatenate([earlier, later, ones], axis=1)
        far_sum = jnp.dot(table, right, preferred_element_type=F32)
        own_keys = qk_ref[here, key_width:] * scale
        own_values = own_half(value_ref[here, :], place_ref[1], share)
        own = lax.dot_general(queries, own_keys, nt, preferred_element_type=F32)
        i = lax.broadcasted_iota(jnp.int32, (rows, rows), 0)
        j = lax.broadcasted_iota(jnp.int32, (rows, rows), 1)
        halves = []
        for d in range(2):
            order = (j <= i) if d == 0 else (j >= i)
            expo = jnp.where(order, near_ref[d, pl.ds(b, 1), :] - top[d], LOW)
            halves.append((own * jnp.exp(expo)).astype(BF))
        lane = lax.broadcasted_iota(jnp.int32, (rows, wide - 2 * share), 1)
        blank = jnp.zeros_like(own_values)
        for d in range(2):
            ones = jnp.where(lane == d, 1.0, 0.0).astype(BF)
            sides = [own_values, blank] if d == 0 else [blank, own_values]
            right = jnp.concatenate(sides + [ones], axis=1)
            far_sum = far_sum + jnp.dot(halves[d], right, preferred_element_type=F32)
        out_ref[here, :] = far_sum

    whole = pl.BlockSpec(memory_space=pltpu.VMEM)
    return pl.pallas_call(
        body,
        grid=(blocks,),
        in_specs=[pl.BlockSpec(memory_space=pltpu.SMEM)] + [whole] * 5,
        out_specs=whole,
        out_shape=jax.ShapeDtypeStruct((length, wide), F32),
        cost_estimate=pl.CostEstimate(
            flops=2 * length * length * (key_width + wide),
            bytes_accessed=4000000,
            transcendentals=length * length,
        ),
    )(place, query_key, values, far, near, columns)


def finish_call(found, coefs, first_memory, first_norm, query_key, local, columns, share):
    z_count, _, key_width = found.shape
    length = query_key.shape[0]
    wide = local.shape[1]

    def body(coef_ref, found_ref, memory_ref, norm_ref, qk_ref, local_ref, col_ref, out_ref, carried):
        normers = []
        for d in range(2):
            state = coef_ref[d, 0] * found_ref[0].astype(F32)
            for k in range(1, z_count):
                state = state + coef_ref[d, k] * found_ref[k].astype(F32)
            start = coef_ref[d, z_count]
            memory = state[:share] + start * memory_ref[d]
            carried[d * share : (d + 1) * share, :] = memory.astype(BF)
            normers.append(
                state[share : share + 1] + state[share + 1 : share + 2] + start * norm_ref[d : d + 1]
            )
        row = lax.broadcasted_iota(jnp.int32, (wide - 2 * share, key_width), 0)
        rest = jnp.zeros((wide - 2 * share, key_width), F32)
        for d in range(2):
            high = normers[d].astype(BF).astype(F32)
            rest = jnp.where(row == d, high, jnp.where(row == 2 + d, normers[d] - high, rest))
        carried[2 * share :, :] = rest.astype(BF)
        reached = lax.dot_general(
            qk_ref[:, :key_width],
            carried[...],
            (((1,), (1,)), ((), ())),
            preferred_element_type=F32,
        )
        total = 0.0
        for d in range(2):
            entry = col_ref[:, 2 + d : 3 + d]
            part = slice(d * share, (d + 1) * share)
            numerator = local_ref[:, part] + entry * reached[:, part]
            one, two = 2 * share + d, 2 * share + 2 + d
            denominator = local_ref[:, one : one + 1] + entry * (
                reached[:, one : one + 1] + reached[:, two : two + 1]
            )
            total = total + numerator / jnp.maximum(jnp.abs(denominator), 1.0)
        out_ref[...] = total.astype(BF)

    whole = pl.BlockSpec(memory_space=pltpu.VMEM)
    return pl.pallas_call(
        body,
        in_specs=[pl.BlockSpec(memory_space=pltpu.SMEM)] + [whole] * 6,
        out_specs=whole,
        out_shape=jax.ShapeDtypeStruct((length, share), BF),
        scratch_shapes=[pltpu.VMEM((wide, key_width), BF)],
        cost_estimate=pl.CostEstimate(
            flops=2 * length * wide * key_width, bytes_accessed=3000000, transcendentals=0
        ),
    )(coefs, found, first_memory, first_norm, query_key, local, columns)


def norm_rows(tokens, gain):
    features = tokens.astype(F32)
    scale = lax.rsqrt(jnp.mean(features * features, axis=1, keepdims=True) + EPS)
    return (features * scale * gain).astype(BF)


def group_tokens(normed, t):
    rows, width = normed.shape
    share = rows // lax.axis_size(TP)
    piece = lax.dynamic_slice_in_dim(normed, t * share, share, 0)
    found = to_each(piece, "y")
    found = to_each(found, "x")
    found = to_each(found, "c")
    found = jnp.transpose(found, (2, 1, 0, 3, 4))
    return found.reshape(-1, width)


def levels(gates, start_level, z, d, per_group):
    chunks, _, rows = gates.shape
    groups = chunks // per_group
    in_gate, forget = gates[:, 0], gates[:, 1]
    p = jnp.arange(rows)
    c = jnp.arange(chunks)
    before = (lambda a, b: a < b) if d == 0 else (lambda a, b: a > b)
    upto = before(p[None, :], p[:, None]) | (p[None, :] == p[:, None])
    cum = jnp.sum(jnp.where(upto[None], forget[:, None, :], 0.0), axis=2)
    total = jnp.sum(forget, axis=1)
    first = in_gate - cum
    tail = total[:, None] - cum + in_gate
    level = jnp.max(tail, axis=1)
    between = before(c[:, None, None], c[None, None, :]) & before(c[None, None, :], c[None, :, None])
    gap = jnp.sum(jnp.where(between, total[None, None, :], 0.0), axis=2)
    earlier = before(c[:, None], c[None, :])
    lead = jnp.sum(jnp.where(earlier, total[:, None], 0.0), axis=0)
    enter = jnp.maximum(
        start_level + lead, jnp.max(jnp.where(earlier, level[:, None] + gap, LOW), axis=0)
    )
    group = c // per_group
    same = group[:, None] == group[None, :]
    rest = jnp.sum(jnp.where(same & before(c[:, None], c[None, :]), total[None, :], 0.0), axis=1)
    group_level = jnp.max((level + rest).reshape(groups, per_group), axis=1)
    g = jnp.arange(groups)
    door = z * per_group + (0 if d == 0 else per_group - 1)
    enter_door = jnp.sum(jnp.where(c == door, enter, 0.0))
    lead_door = jnp.sum(jnp.where(c == door, lead, 0.0))
    middle = before(g[:, None], group[None, :]) & before(group[None, :], z)
    group_gap = jnp.sum(jnp.where(middle, total[None, :], 0.0), axis=1)
    coef = jnp.where(
        before(g, z), jnp.exp(jnp.where(before(g, z), group_level + group_gap - enter_door, LOW)), 0.0
    )
    start_coef = jnp.exp(start_level + lead_door - enter_door)

    def own(values):
        return lax.dynamic_slice_in_dim(values, z * per_group, per_group, 0)

    def own2(values):
        return lax.dynamic_slice(
            values, (z * per_group, z * per_group), (per_group, per_group)
        )

    first_own, tail_own, enter_own = own(first), own(tail), own(enter)
    peak = jnp.max(jnp.where(upto[None], first_own[:, None, :], LOW), axis=2)
    top = jnp.maximum(enter_own[:, None], peak)
    o = jnp.arange(per_group)
    from_door = jnp.sum(
        jnp.where(before(o[:, None], o[None, :]), own(total)[:, None], 0.0), axis=0
    )
    entry = jnp.exp((from_door + enter_door)[:, None] - top)
    own_group = jnp.sum(jnp.where(g == z, group_level, 0.0))
    state_weight = jnp.exp(tail_own + own(rest)[:, None] - own_group)
    seen = tail_own[:, None, :] + own2(gap)[:, :, None]
    seen = jnp.transpose(seen, (1, 0, 2)).reshape(per_group, per_group * rows)
    return seen, first_own, top.reshape(-1), entry.reshape(-1), state_weight.reshape(-1), coef, start_coef


def layer(
    tokens,
    norm_gain,
    conv_value_weight,
    conv_gate_weight,
    conv_kernel,
    conv_bias,
    channel_gain,
    query_weight,
    key_weight,
    value_weight,
    gate_weight,
    gate_offset,
    start_memory,
    start_norm,
    start_level,
    cell_gain,
    out_conv_weight,
    out_cell_weight,
):
    z, y, t = lax.axis_index("z"), lax.axis_index("y"), lax.axis_index(TP)
    z_count, y_count, t_count = lax.axis_size("z"), lax.axis_size("y"), lax.axis_size(TP)
    rows = tokens.shape[0]
    chan = conv_kernel.shape[1]
    key_width = start_norm.shape[2]
    value_width = start_memory.shape[2]
    share = value_width // y_count
    channels = chan * t_count

    weights = side_by_side(
        (
            query_weight,
            key_weight,
            conv_value_weight,
            conv_gate_weight,
            value_weight,
            out_conv_weight,
            out_cell_weight,
        )
    )
    weights = lax.all_gather(weights, SP, axis=0, tiled=True)
    conv_at = 2 * key_width
    value_at = conv_at + 2 * chan
    out_at = value_at + value_width

    normed = norm_rows(tokens, norm_gain)

    heads = gate_weight.shape[1] // 4
    gate_pre = jnp.dot(normed, gate_weight, preferred_element_type=F32)
    mine = jnp.arange(heads) == t
    gate_pre = jnp.sum(
        jnp.where(mine, gate_pre.reshape(rows, 4, heads), 0.0), axis=2
    ).T.reshape(2, 2, rows)
    gate_pre = gate_pre + gate_offset[:, :, 0]
    gates = jnp.stack([gate_pre[:, 0], jax.nn.log_sigmoid(gate_pre[:, 1])], axis=1)
    gates = to_each(gates.reshape(4, rows), SP).reshape(-1, 2, 2, rows)

    half = conv_kernel.shape[0] // 2
    pad = 16
    count = z_count * y_count
    up = [(i, i + 1) for i in range(count - 1)]
    down = [(i + 1, i) for i in range(count - 1)]
    above = lax.ppermute(normed[rows - pad :], SP, up)
    below = lax.ppermute(normed[:pad], SP, down)
    around = jnp.concatenate([above, normed, below], axis=0)

    group = group_tokens(normed, t)
    plans = [levels(gates[:, d], start_level[d, 0], z, d, y_count) for d in range(2)]

    step = jnp.arange(y_count)[:, None]
    chunk_of = (jnp.arange(y_count * rows) // rows)[None, :]
    far = jnp.where(
        chunk_of < step, plans[0][0], jnp.where(chunk_of > step, plans[1][0], LOW)
    )
    near = jnp.stack([plans[0][1], plans[1][1]])
    columns = jnp.stack(
        [plans[d][k] for k in (2, 3, 4) for d in range(2)] + [plans[0][2]] * 2, axis=1
    )
    coefs = jnp.stack([jnp.append(plans[d][5], plans[d][6]) for d in range(2)])
    first_memory = lax.dynamic_slice_in_dim(start_memory[:, 0], y * share, share, 1)
    first_norm = start_norm[:, 0]

    pair = lax.dynamic_slice_in_dim(weights, value_at + (y // 2) * 2 * share, 2 * share, 1)
    query_key = jnp.dot(group, weights[:, :conv_at], preferred_element_type=F32).astype(BF)
    values = jnp.dot(group, pair, preferred_element_type=F32).astype(BF)
    place = jnp.stack([z, y % 2])
    sent = states_call(place, query_key, values, columns, share, z_count)
    found = exchange(sent, "z")
    around, sent = lax.optimization_barrier((around, sent))
    local = local_call(place, query_key, values, far, near, columns, share, y_count)

    conv_both = jnp.dot(around, weights[:, conv_at:value_at], preferred_element_type=F32).astype(BF).astype(F32)
    gated = (conv_both[:, :chan] * jax.nn.sigmoid(conv_both[:, chan:])).astype(BF).astype(F32)
    shift = pad - half
    conv = conv_bias + sum(
        conv_kernel[j] * gated[shift + j : shift + j + rows] for j in range(conv_kernel.shape[0])
    )
    stats = jnp.stack([jnp.sum(conv, axis=1), jnp.sum(conv * conv, axis=1)])
    stats = lax.all_gather(stats, TP)
    stats = jnp.sum(stats, axis=0) / channels
    mean, var = stats[0], stats[1] - stats[0] * stats[0]
    conv_out = jax.nn.silu(
        (conv - mean[:, None]) * lax.rsqrt(var + EPS)[:, None] * channel_gain
    ).astype(BF)

    cell = finish_call(found, coefs, first_memory, first_norm, query_key, local, columns, share)
    cell = cell.reshape(y_count, rows, share)
    cell = exchange(cell, "y")
    cell = jnp.transpose(cell, (1, 0, 2)).reshape(rows, value_width).astype(F32)
    cell_out = (
        cell * lax.rsqrt(jnp.mean(cell * cell, axis=1, keepdims=True) + EPS) * cell_gain
    ).astype(BF)

    features = jnp.concatenate([conv_out, cell_out], axis=1)
    partial = lax.dot_general(
        features, weights[:, out_at:], (((1,), (1,)), ((), ())), preferred_element_type=F32
    ).astype(BF)
    partial = lax.all_to_all(
        partial.reshape(t_count, rows // t_count, -1), TP, 0, 0, tiled=True
    )
    return jnp.sum(partial.astype(F32), axis=0).astype(BF)


def solution(mesh):
    z, y, x, c = mesh_shape(mesh)
    split = Mesh(mesh.devices.reshape(z, y, x, c), ("z", "y", "x", "c"))
    return jax.shard_map(
        layer,
        mesh=split,
        in_specs=(
            P(SP, None),
            P(),
            P(SP, TP),
            P(SP, TP),
            P(None, TP),
            P(TP),
            P(TP),
            P(SP, TP),
            P(SP, TP),
            P(SP, TP),
            P(),
            P(None, None, TP, SP),
            P(None, TP, None, None),
            P(None, TP, None),
            P(None, TP),
            P(TP),
            P(SP, TP),
            P(SP, TP),
        ),
        out_specs=P(SP + TP, None),
        check_vma=False,
    )


def mesh_shape(mesh):
    return 8, 8, mesh.shape["tp"] // 2, 2
```
